128 devices in a mesh: fs: 32 (over z, y, core), tp: 4 (over x).
Axes of the slice: x: 4, y: 4, z: 4, core: 2. Of those that a mesh axis runs over, the one named last changes fastest.
Arguments:
- inputs: bfloat16 [65536, 2048], P('fs'), may hold values from -6 to 6
- attn_out: bfloat16 [65536, 1024], P('fs', 'tp'), may hold values from -6 to 6
- grad_query: bfloat16 [65536, 1024], P('fs', 'tp'), may hold values from -0.0625 to 0.0625
- grad_key: bfloat16 [65536, 1024], P('fs', 'tp'), may hold values from -0.0625 to 0.0625
- grad_mixed: bfloat16 [65536, 2048], P('fs'), may hold values from -0.109375 to 0.109375
- query_weight: float32 [2048, 1024], P('fs', 'tp'), may hold values from -0.75 to 0.75
- key_weight: float32 [2048, 1024], P('fs', 'tp'), may hold values from -0.75 to 0.75
- out_weight: float32 [1024, 2048], P('tp', 'fs'), may hold values from -0.75 to 0.75
- factors: bfloat16 [3, 2048, 256], P(None, 'fs'), may hold values from -0.125 to 0.125
- moment_first: float32 [3, 256, 1024], P(None, 'fs', 'tp'), may hold values from -6 to 6
- moment_second: float32 [3, 256, 1024], P(None, 'fs', 'tp'), may hold values from 0.05 to 2
Outputs:
- step_query: float32 [2048, 1024], P('fs', 'tp')
- step_key: float32 [2048, 1024], P('fs', 'tp')
- step_out: float32 [1024, 2048], P('tp', 'fs')
- copy_query: bfloat16 [2048, 1024], P(None, 'tp')
- copy_key: bfloat16 [2048, 1024], P(None, 'tp')
- copy_out: bfloat16 [1024, 2048], P('tp')
- first_new: float32 [3, 256, 1024], P(None, 'fs', 'tp')
- second_new: float32 [3, 256, 1024], P(None, 'fs', 'tp')
The draws below stay inside these ranges and needn't reach their ends.
All inputs are finite; a program needn't handle non-finite values.
Results may differ from the reference program's by a relative error of at most 0.006.
Values may be sent and summed in bfloat16 or wider, within the bound.
A program may use at most 128 MiB of HBM per device.

```python
import math
import jax
import jax.numpy as jnp
from jax import lax

D = 2048
RANK = 256
TOKENS = 65536
HW = 1024


def spiked(values, key, source, target, blocks, factor):
    owner, partner = [(jnp.arange(values.shape[dim]) // (values.shape[dim] // blocks)).reshape([-1 if axis == dim else 1 for axis in range(values.ndim)]) for dim in (source, target)]
    chosen = jax.random.permutation(key, blocks)[partner]
    strong = (owner == chosen) | (owner == (partner + blocks // 2) % blocks)
    return jnp.where(strong, factor * values, values)


def levels(rng, dims, split, smallest, top_value):
    level, own = 1.0, jax.random.fold_in(rng, 6)
    for position, blocks in split:
        draws = jnp.exp(jax.random.uniform(jax.random.fold_in(own, position), (blocks,), jnp.float32, smallest / len(split), top_value / len(split)))
        level = level * jnp.repeat(draws, dims[position] // blocks).reshape([-1 if axis == position else 1 for axis in range(len(dims))])
    return level


def centred(rng, shape, spread, most, shards=(), held_as=jnp.bfloat16):
    entries = jax.random.normal(rng, shape, jnp.float32) * spread
    if len(shards) > 0:
        entries = levels(rng, shape, shards, -0.22, 0.18) * entries
    return jnp.clip(entries, min=-most, max=most).astype(held_as)


def noise_with(own_key, extent, scale, bound, shards, heavy, dtype=jnp.bfloat16):
    result = scale * jax.random.normal(own_key, extent, jnp.float32)
    if shards:
        result = result * levels(own_key, extent, shards, -0.22, 0.18)
    return jnp.clip(spiked(result, jax.random.fold_in(own_key, 3), *heavy), -bound, bound).astype(dtype)


def setup_inputs(seed: int = 0) -> dict:
    key_of = jax.random.split(jax.random.key(seed), 12)
    inputs = noise_with(key_of[0], (TOKENS, D), 1.0, 6.0, ((0, 32),), (0, 1, 32, 2.75))
    attn_out = centred(key_of[1], (TOKENS, HW), 1.0, 6.0, ((0, 32), (1, 4)))
    grad_query = centred(key_of[2], (TOKENS, HW), (1.0 / TOKENS ** 0.5), 0.0625, ((0, 32), (1, 4)))
    grad_key = centred(key_of[3], (TOKENS, HW), (1.0 / TOKENS ** 0.5), 0.0625, ((0, 32), (1, 4)))
    grad_mixed = noise_with(key_of[4], (TOKENS, D), (1.0 / TOKENS ** 0.5), 0.109375, ((0, 32),), (0, 1, 32, 2.75))
    query_weight = centred(key_of[5], (D, HW), 0.05, 0.75, ((0, 32), (1, 4)), jnp.float32)
    key_weight = centred(key_of[6], (D, HW), 0.05, 0.75, ((0, 32), (1, 4)), jnp.float32)
    out_weight = centred(key_of[7], (HW, D), 0.05, 0.75, ((0, 4), (1, 32)), jnp.float32)
    factors = centred(key_of[8], (3, D, RANK), D ** -0.5, 0.125, ((1, 32),))
    moment_first = noise_with(key_of[9], (3, RANK, HW), 1.0, 6.0, ((1, 32), (2, 4)), (1, 2, 32, 2.75), jnp.float32)
    moment_second = jnp.clip(jnp.exp(math.log(2.0) - 3.6888794 * jax.random.uniform(key_of[10], (3, RANK, HW), jnp.float32) ** levels(key_of[10], (3, RANK, HW), ((1, 32), (2, 4)), -0.2, 0.2)), 0.05, 2.0)
    return {"inputs": inputs, "attn_out": attn_out, "grad_query": grad_query, "grad_key": grad_key, "grad_mixed": grad_mixed, "query_weight": query_weight, "key_weight": key_weight, "out_weight": out_weight, "factors": factors, "moment_first": moment_first, "moment_second": moment_second}


first_decay = 0.8
second_decay = 0.9
epsilon = 1e-08
learn_rate = 0.02

def project(left_side, right_side, factor_rows):
    mapped = jnp.dot(left_side.astype(jnp.float32), factor_rows.astype(jnp.float32), precision=lax.Precision.HIGHEST)
    return jnp.dot(mapped.T, right_side.astype(jnp.float32), precision=lax.Precision.HIGHEST)

def widen_product(left_side, right_side):
    return jnp.dot(left_side.astype(jnp.float32), right_side.astype(jnp.float32), precision=lax.Precision.HIGHEST)

def reference(inputs, attn_out, grad_query, grad_key, grad_mixed, query_weight, key_weight, out_weight, factors, moment_first, moment_second):
    projected = jnp.stack([project(inputs, grad_query, factors[0]), project(inputs, grad_key, factors[1]), project(grad_mixed, attn_out, factors[2])])
    first_new = first_decay * moment_first + (1.0 - first_decay) * projected
    second_new = second_decay * moment_second + (1.0 - second_decay) * projected * projected
    ratio = first_new / (jnp.sqrt(second_new) + epsilon)
    square_total = jnp.sum(ratio * ratio)
    step_scale = lax.rsqrt(square_total / (3 * RANK * HW) + 1.0)
    ratio_b = ratio.astype(jnp.bfloat16)
    step_query = step_scale * widen_product(factors[0], ratio_b[0])
    step_key = step_scale * widen_product(factors[1], ratio_b[1])
    step_out = step_scale * widen_product(factors[2], ratio_b[2]).T
    copy_query = (query_weight - learn_rate * step_query).astype(jnp.bfloat16)
    copy_key = (key_weight - learn_rate * step_key).astype(jnp.bfloat16)
    copy_out = (out_weight - learn_rate * step_out).astype(jnp.bfloat16)
    return (step_query, step_key, step_out, copy_query, copy_key, copy_out, first_new, second_new)
```

```python
import jax
import jax.numpy as jnp
from jax import lax
from jax.experimental import pallas as pl
from jax.experimental.pallas import tpu as pltpu
from jax.sharding import Mesh
from jax.sharding import PartitionSpec as P

RANK = 256
HW = 1024
FS = ("z", "y", "c")
MESH = pl.DeviceIdType.MESH
bf16 = jnp.bfloat16
f32 = jnp.float32

first_decay = 0.8
second_decay = 0.9
epsilon = 1e-08
learn_rate = 0.02

ROUNDS = (
    ((0, 1), (0, 3), (1, 0), (3, 0)),
    ((1, 1), (1, 3), (3, 1), (3, 3), (0, 2), (2, 0)),
    ((1, 2), (3, 2), (2, 1), (2, 3)),
    ((2, 2),),
)


def wrap(v):
    return lax.rem(v, 4)


class Gather:
    def __init__(self, buf, recv, send, pair_recv, pair_send, where):
        self.buf, self.recv, self.send = buf, recv, send
        self.pair_recv, self.pair_send, self.where = pair_recv, pair_send, where
        self.started = []
        self.count = [0, 0]

    def device(self, dz, dy, other=False):
        z, y, c, x = self.where
        return (wrap(z + dz), wrap(y + dy), 1 - c if other else c, x)

    def block(self, a, b, half, quarter):
        z, y, c, x = self.where
        dz, dy = (b, a) if half == 0 else (a, b)
        zs, ys = wrap(z + 4 - dz), wrap(y + 4 - dy)
        start, size = (32 * half, 32) if quarter is None else (32 * half + 16 * quarter, 16)
        return self.buf.at[:, zs, ys, c, pl.ds(start, size)], (half, zs, ys, quarter or 0)

    def copy(self, a, b, half, quarter, to, other=False):
        ref, index = self.block(a, b, half, quarter)
        recv = self.pair_recv if other else self.recv
        sems = self.pair_send if other else self.send
        n = self.count[other]
        self.count[other] += 1
        cp = pltpu.make_async_remote_copy(
            src_ref=ref,
            dst_ref=ref,
            send_sem=sems.at[n],
            recv_sem=recv.at[index[:3]] if other else recv.at[index],
            device_id=to,
            device_id_type=MESH,
        )
        cp.start()
        self.started.append(cp)

    def steps(self, half, dim, amount):
        moves_y = (dim == 0) == (half == 0)
        return self.device(0, amount) if moves_y else self.device(amount, 0)

    def wait(self, a, b, half, quarter):
        ref, index = self.block(a, b, half, quarter)
        pltpu.make_async_remote_copy(
            src_ref=ref,
            dst_ref=ref,
            send_sem=self.send.at[0],
            recv_sem=self.recv.at[index],
            device_id=self.where,
            device_id_type=MESH,
        ).wait_recv()

    def own(self):
        for half in range(2):
            for dim in range(2):
                self.copy(0, 0, half, None, self.steps(half, dim, 1))
                self.copy(0, 0, half, None, self.steps(half, dim, 3))
        for half in range(2):
            self.copy(0, 0, half, None, self.device(0, 0, True), True)

    def round(self, number):
        for a, b in ROUNDS[number]:
            for half in range(2):
                if b == 2 or (b == 0 and a == 2):
                    self.wait(a, b, half, 0)
                    self.wait(a, b, half, 1)
                else:
                    self.wait(a, b, half, None)
                if b == 0:
                    if a == 1:
                        self.copy(a, b, half, 0, self.steps(half, 0, 1))
                    if a == 3:
                        self.copy(a, b, half, 1, self.steps(half, 0, 3))
                    self.copy(a, b, half, None, self.steps(half, 1, 1))
                    self.copy(a, b, half, None, self.steps(half, 1, 3))
                elif b == 1:
                    self.copy(a, b, half, 0, self.steps(half, 1, 1))
                elif b == 3:
                    self.copy(a, b, half, 1, self.steps(half, 1, 3))
                self.copy(a, b, half, None, self.device(0, 0, True), True)

    def from_pair(self):
        z, y, c, x = self.where
        for half in range(2):
            for zs in range(4):
                for ys in range(4):
                    ref = self.buf.at[:, zs, ys, 1 - c, pl.ds(32 * half, 32)]
                    pltpu.make_async_remote_copy(
                        src_ref=ref,
                        dst_ref=ref,
                        send_sem=self.send.at[0],
                        recv_sem=self.pair_recv.at[half, zs, ys],
                        device_id=self.where,
                        device_id_type=MESH,
                    ).wait_recv()

    def finish(self):
        for cp in self.started:
            cp.wait_send()


def exchange_kernel(
    inputs, attn_out, grad_query, grad_key, grad_mixed, query_weight, key_weight, out_weight, factors, moment_first, moment_second,
    fg, wg, rg, first_new, second_new, squares,
    left, right, right_t, grad_t, weights, old_first, old_second, partial, from_core, chip_sum, arrived, sq_arrived,
    f_recv, f_send, f_pair_recv, f_pair_send,
    w_recv, w_send, w_pair_recv, w_pair_send,
    p_pair, p_recv, p_send, r_recv, r_send, r_pair, sq_recv, sq_send,
    local, left_sem, right_sem,
):
    z, y, c, x = where = tuple(lax.axis_index(a) for a in ("z", "y", "c", "x"))
    chip = z * 4 + y
    partner = (z, y, 1 - c, x)

    barrier = pltpu.get_barrier_semaphore()
    greeted = [
        (wrap(z + 1), y, c, x), (wrap(z + 3), y, c, x), (z, wrap(y + 1), c, x), (z, wrap(y + 3), c, x), partner,
        (z, y, c, wrap(x + 1)), (z, y, c, wrap(x + 2)), (z, y, c, wrap(x + 3)),
    ]
    for other in greeted:
        pl.semaphore_signal(barrier, inc=1, device_id=other, device_id_type=MESH)

    own_factors = pltpu.make_async_copy(factors, fg.at[:, z, y, c], local.at[0])
    own_factors.start()
    right_loads = []
    for m, ref in enumerate((grad_query, grad_key, attn_out)):
        right_loads.append(pltpu.make_async_copy(ref, right.at[m], right_sem.at[m]))
    left_loads = []
    for m, ref in enumerate((inputs, grad_mixed)):
        for n in range(4):
            columns = pl.ds(512 * n, 512)
            left_loads.append(pltpu.make_async_copy(ref.at[:, columns], left.at[m, n], left_sem.at[m, n]))
    small = [
        pltpu.make_async_copy(query_weight, weights.at[0], local.at[1]),
        pltpu.make_async_copy(key_weight, weights.at[1], local.at[2]),
        pltpu.make_async_copy(out_weight, weights.at[2], local.at[3]),
        pltpu.make_async_copy(moment_first, old_first, local.at[4]),
        pltpu.make_async_copy(moment_second, old_second, local.at[5]),
    ]
    right_loads[0].start()
    right_loads[1].start()
    for cp in small:
        cp.start()
    left_loads[0].start()
    left_loads[1].start()
    right_loads[2].start()
    for cp in left_loads[2:]:
        cp.start()

    pl.semaphore_wait(barrier, len(greeted))
    own_factors.wait()
    gf = Gather(fg, f_recv, f_send, f_pair_recv, f_pair_send, where)
    gw = Gather(wg, w_recv, w_send, w_pair_recv, w_pair_send, where)
    gf.own()

    for cp in small:
        cp.wait()
    wg[0, z, y, c] = weights[0].astype(bf16)
    wg[1, z, y, c] = weights[1].astype(bf16)
    wg[2, z, y, c] = weights[2].astype(bf16)

    def turn(m):
        right_loads[m].wait()
        for n in range(4):
            rows = pl.ds(512 * n, 512)
            right_t[pl.ds(256 * m, 256), rows] = right[m, rows, :].T

    def query_key(n):
        left_loads[n].wait()
        for h in range(2):
            product = jnp.dot(right_t[0:512, :], left[0, n, :, 256 * h : 256 * h + 256], preferred_element_type=f32)
            grad_t[0:512, 512 * n + 256 * h : 512 * n + 256 * h + 256] = product.astype(bf16)

    def output(n):
        left_loads[4 + n].wait()
        product = jnp.dot(right_t[512:768, :], left[1, n], preferred_element_type=f32)
        grad_t[512:768, 512 * n : 512 * n + 512] = product.astype(bf16)

    turn(0)
    turn(1)
    query_key(0)
    gf.round(0)
    query_key(1)
    query_key(2)
    gf.round(1)
    gw.own()
    query_key(3)
    turn(2)
    output(0)
    gf.round(2)
    output(1)
    output(2)
    gf.round(3)
    gw.round(0)
    output(3)
    gf.from_pair()

    for m in range(3):
        projected = jnp.dot(grad_t[256 * m : 256 * m + 256, :], fg[m].reshape(2048, RANK), preferred_element_type=f32)
        projected = projected.T.reshape(32, 8, 256)
        packed = jnp.concatenate([projected[:, :, :128], projected[:, :, 128:]], axis=1).astype(bf16)
        partial[:, :, :, 128 * m : 128 * m + 128] = packed.reshape(16, 2, 16, 128)

    pair_copy = pltpu.make_async_remote_copy(
        src_ref=partial.at[:, 1 - c], dst_ref=from_core, send_sem=p_pair.at[0], recv_sem=p_pair.at[1],
        device_id=partner, device_id_type=MESH,
    )
    pair_copy.start()
    gw.round(1)
    pair_copy.wait_recv()
    chip_sum[...] = (partial[:, c].astype(f32) + from_core[...].astype(f32)).astype(bf16)

    offsets = [(dz, dy) for dz in range(4) for dy in range(4) if (dz, dy) != (0, 0)]
    offsets.sort(key=lambda o: -(min(o[0], 4 - o[0]) + min(o[1], 4 - o[1])))
    p_copies = []
    for k, (dz, dy) in enumerate(offsets):
        tz, ty = wrap(z + dz), wrap(y + dy)
        cp = pltpu.make_async_remote_copy(
            src_ref=chip_sum.at[tz * 4 + ty], dst_ref=arrived.at[k], send_sem=p_send.at[k], recv_sem=p_recv.at[k],
            device_id=(tz, ty, c, x), device_id_type=MESH,
        )
        cp.start()
        p_copies.append(cp)
    gw.round(2)
    total = chip_sum[chip].astype(f32)
    for k in reversed(range(15)):
        p_copies[k].wait_recv()
        total = total + arrived[k].astype(f32)

    ratios = []
    for m in range(3):
        lanes = slice(128 * m, 128 * m + 128)
        p = jnp.concatenate([total[0:8, lanes], total[8:16, lanes]], axis=1)
        first = first_decay * old_first[m] + (1.0 - first_decay) * p
        second = second_decay * old_second[m] + (1.0 - second_decay) * p * p
        first_new[m] = first
        second_new[m] = second
        ratio = first / (jnp.sqrt(second) + epsilon)
        ratios.append(jnp.concatenate([ratio[:, :128], ratio[:, 128:]], axis=0))
    rg[chip, c] = jnp.concatenate(ratios, axis=1).astype(bf16)

    r_copies = []
    for k, (dz, dy) in enumerate(offsets):
        tz, ty = wrap(z + dz), wrap(y + dy)
        r_copies.append(
            pltpu.make_async_remote_copy(
                src_ref=rg.at[chip, c], dst_ref=rg.at[chip, c], send_sem=r_send.at[k], recv_sem=r_recv.at[k],
                device_id=(tz, ty, c, x), device_id_type=MESH,
            )
        )
        r_copies[-1].start()
    gw.round(3)
    for k, (dz, dy) in enumerate(offsets):
        source = wrap(z + 4 - dz) * 4 + wrap(y + 4 - dy)
        pltpu.make_async_remote_copy(
            src_ref=rg.at[source, c], dst_ref=rg.at[source, c], send_sem=r_send.at[k], recv_sem=r_recv.at[k],
            device_id=where, device_id_type=MESH,
        ).wait_recv()
    r_forward = pltpu.make_async_remote_copy(
        src_ref=rg.at[:, c], dst_ref=rg.at[:, c], send_sem=r_pair.at[0], recv_sem=r_pair.at[1],
        device_id=partner, device_id_type=MESH,
    )
    r_forward.start()
    gw.from_pair()
    pltpu.make_async_remote_copy(
        src_ref=rg.at[:, 1 - c], dst_ref=rg.at[:, 1 - c], send_sem=r_pair.at[0], recv_sem=r_pair.at[1],
        device_id=partner, device_id_type=MESH,
    ).wait_recv()

    everyone = rg[...].astype(f32)
    squared = jnp.sum((everyone * everyone).reshape(64, 8, 384), axis=0)
    sq_arrived[0] = squared[:, :128] + squared[:, 128:256] + squared[:, 256:]
    s_copies = []
    for k in range(1, 4):
        s_copies.append(
            pltpu.make_async_remote_copy(
                src_ref=sq_arrived.at[0], dst_ref=sq_arrived.at[k], send_sem=sq_send.at[k - 1], recv_sem=sq_recv.at[k - 1],
                device_id=(z, y, c, wrap(x + k)), device_id_type=MESH,
            )
        )
        s_copies[-1].start()
    for cp in s_copies:
        cp.wait_recv()
    squares[...] = sq_arrived[0] + sq_arrived[1] + sq_arrived[2] + sq_arrived[3]

    gf.finish()
    gw.finish()
    pair_copy.wait_send()
    r_forward.wait_send()
    for cp in p_copies + r_copies + s_copies:
        cp.wait_send()


def step_kernel(
    fg, wg, rg, first_in, second_in, squares, factors,
    step_query, step_key, step_out, copy_query, copy_key, copy_out, first_new, second_new, ratios,
):
    i = pl.program_id(0)
    scale = lax.rsqrt(jnp.sum(squares[...], keepdims=True) / (3 * RANK * HW) + 1.0)

    @pl.when(i == 0)
    def _():
        first_new[...] = first_in[...]
        second_new[...] = second_in[...]
        for m in range(3):
            part = rg[:, :, :, 128 * m : 128 * m + 128].astype(f32).reshape(32, 16, 128)
            whole = jnp.concatenate([part[:, :8], part[:, 8:]], axis=2).reshape(RANK, 256)
            ratios[m] = whole.astype(bf16)
        ratios[3] = whole.T.astype(bf16)
        for m, out in enumerate((step_query, step_key, step_out)):
            out[...] = scale * jnp.dot(factors[m], ratios[m], preferred_element_type=f32)

    rate = learn_rate * scale
    for m, out in ((0, copy_query), (1, copy_key)):
        change = jnp.dot(fg[m, i].reshape(512, RANK), ratios[m], preferred_element_type=f32)
        out[...] = (wg[m, i].reshape(512, 256).astype(f32) - rate * change).astype(bf16)
    change = lax.dot_general(ratios[3], fg[2, i].reshape(512, RANK), (((1,), (1,)), ((), ())), preferred_element_type=f32)
    copy_out[...] = (wg[2, i].reshape(512, 256).astype(f32).T - rate * change).astype(bf16)


def per_device(*args):
    sem = pltpu.SemaphoreType.DMA
    vmem = pl.BlockSpec(memory_space=pltpu.VMEM)
    args = list(args)
    args[7] = args[7].T
    held = [pltpu.with_memory_space_constraint(a, pltpu.HBM) for a in args]
    outs = pl.pallas_call(
        exchange_kernel,
        out_shape=(
            pltpu.VMEM((3, 4, 4, 2, 64, 256), bf16),
            pltpu.VMEM((3, 4, 4, 2, 64, 256), bf16),
            pltpu.VMEM((16, 2, 16, 384), bf16),
            pltpu.VMEM((3, 8, 256), f32),
            pltpu.VMEM((3, 8, 256), f32),
            pltpu.VMEM((8, 128), f32),
        ),
        in_specs=[pl.BlockSpec(memory_space=pltpu.HBM)] * 11,
        out_specs=(vmem,) * 6,
        scratch_shapes=[
            pltpu.VMEM((2, 4, 2048, 512), bf16),
            pltpu.VMEM((3, 2048, 256), bf16),
            pltpu.VMEM((768, 2048), bf16),
            pltpu.VMEM((768, 2048), bf16),
            pltpu.VMEM((3, 64, 256), f32),
            pltpu.VMEM((3, 8, 256), f32),
            pltpu.VMEM((3, 8, 256), f32),
            pltpu.VMEM((16, 2, 16, 384), bf16),
            pltpu.VMEM((16, 16, 384), bf16),
            pltpu.VMEM((16, 16, 384), bf16),
            pltpu.VMEM((15, 16, 384), bf16),
            pltpu.VMEM((4, 8, 128), f32),
            sem((2, 4, 4, 2)), sem((40,)), sem((2, 4, 4)), sem((32,)),
            sem((2, 4, 4, 2)), sem((40,)), sem((2, 4, 4)), sem((32,)),
            sem((2,)), sem((15,)), sem((15,)), sem((15,)), sem((15,)), sem((2,)), sem((3,)), sem((3,)),
            sem((6,)), sem((2, 4)), sem((3,)),
        ],
        compiler_params=pltpu.CompilerParams(collective_id=0, has_side_effects=True, vmem_limit_bytes=44 << 20),
        name="exchange",
    )(*held)
    fg, wg, rg, first_new, second_new, squares = [pltpu.with_memory_space_constraint(o, pltpu.VMEM) for o in outs]
    whole = lambda *shape: pl.BlockSpec(shape, lambda i: (0,) * len(shape))
    outs = pl.pallas_call(
        step_kernel,
        grid=(4,),
        in_specs=[vmem] * 7,
        out_specs=(
            whole(64, 256),
            whole(64, 256),
            whole(64, 256),
            pl.BlockSpec((512, 256), lambda i: (i, 0)),
            pl.BlockSpec((512, 256), lambda i: (i, 0)),
            pl.BlockSpec((256, 512), lambda i: (0, i)),
            whole(3, 8, 256),
            whole(3, 8, 256),
        ),
        out_shape=(
            jax.ShapeDtypeStruct((64, 256), f32),
            jax.ShapeDtypeStruct((64, 256), f32),
            jax.ShapeDtypeStruct((64, 256), f32),
            jax.ShapeDtypeStruct((2048, 256), bf16),
            jax.ShapeDtypeStruct((2048, 256), bf16),
            jax.ShapeDtypeStruct((256, 2048), bf16),
            jax.ShapeDtypeStruct((3, 8, 256), f32),
            jax.ShapeDtypeStruct((3, 8, 256), f32),
        ),
        scratch_shapes=[pltpu.VMEM((4, 256, 256), bf16)],
        compiler_params=pltpu.CompilerParams(vmem_limit_bytes=32 << 20),
        name="steps",
    )(fg, wg, rg, first_new, second_new, squares, args[8])
    return (*outs[:2], outs[2].T, *outs[3:])


def solution(mesh):
    split = Mesh(mesh.devices.reshape(4, 4, 2, mesh.shape["tp"]), ("z", "y", "c", "x"))
    placed = (
        P(FS, None),
        P(FS, "x"),
        P(FS, "x"),
        P(FS, "x"),
        P(FS, None),
        P(FS, "x"),
        P(FS, "x"),
        P("x", FS),
        P(None, FS, None),
        P(None, FS, "x"),
        P(None, FS, "x"),
    )
    return jax.shard_map(
        per_device,
        mesh=split,
        in_specs=placed,
        out_specs=(
            P(FS, "x"),
            P(FS, "x"),
            P("x", FS),
            P(None, "x"),
            P(None, "x"),
            P("x", None),
            P(None, FS, "x"),
            P(None, FS, "x"),
        ),
        check_vma=False,
    )
```
